32 devices in a mesh: sp: 8 (over z, x), tp: 4 (over y, core).
Axes of the slice: x: 2, y: 2, z: 4, core: 2. Of those that a mesh axis runs over, the one named last changes fastest.
Arguments:
- block_input: bfloat16 [2048, 2048], P('sp'), may hold values from -8 to 8
- queries: bfloat16 [2048, 1024], P('sp', 'tp'), may hold values from -6 to 6
- keys: bfloat16 [2048, 1024], P('sp', 'tp'), may hold values from -6 to 6
- w_value: bfloat16 [2048, 2048], P(None, 'tp'), may hold values from -0.125 to 0.125
- log_decay: float32 [2048, 1024], P('sp', 'tp'), as said below
- d_out: bfloat16 [2048, 2048], P('sp', 'tp'), may hold values from -0.125 to 0.125
Outputs:
- d_queries: bfloat16 [2048, 1024], P('sp', 'tp')
- d_keys: bfloat16 [2048, 1024], P('sp', 'tp')
- d_log_decay: float32 [2048, 1024], P('sp', 'tp')
- d_w_value: float32 [2048, 2048], P('sp', 'tp')
- row_norms: float32 [2048], P('sp')
The draws below stay inside these ranges and needn't reach their ends.
Inputs may be any that keep to these rules, and one draw needn't show every extreme that they name: log_decay is negative; key channels differ in rate, and rates change along the sequence.
All inputs are finite; a program needn't handle non-finite values.
Results may differ from the reference program's by a relative error of at most 0.015.
Values sent between devices are 32-bit elements; how exact they have to be, the bound alone decides.
A program may use at most 64 MiB of HBM per device.

```python
import math
import jax
import jax.numpy as jnp
from jax import lax

D = 2048
HEADS = 8
DK = 128
DV = 256
TOK_DEV = 256
TOKENS = 2048


def draw_log_decay(key, part):
    rate_key, noise_key, span_key = jax.random.split(jax.random.fold_in(key, 11), 3)
    rates = jnp.exp(jax.random.uniform(rate_key, (HEADS * DK,), jnp.float32, math.log(0.08), math.log(2.1))) / TOKENS
    span_factor = jnp.exp(jax.random.uniform(span_key, (TOKENS // TOK_DEV, 1, HEADS * DK), jnp.float32, -1.5, 1.5))
    span_factor = jnp.broadcast_to(span_factor, (TOKENS // TOK_DEV, TOK_DEV, HEADS * DK)).reshape(TOKENS, HEADS * DK)
    noise = jnp.clip(0.5 * jax.random.normal(noise_key, (TOKENS, HEADS * DK), jnp.float32), -1.5, 1.5)
    return (-rates[None, :] * span_factor * jnp.exp(noise)).astype(jnp.float32)


def strengthened(values, key, source, target, shards_of, factor):
    def block_of(position):
        return (jnp.arange(values.shape[position]) // (values.shape[position] // shards_of)).reshape((-1,) + (1,) * (values.ndim - 1 - position))

    near = jax.random.permutation(key, shards_of)[block_of(target)]
    other_side = (block_of(target) + shards_of // 2) % shards_of
    return jnp.where((block_of(source) == near) | (block_of(source) == other_side), factor * values, values)


def levels(own_key, extent, shards, least, top_value):
    loudness, own = 1.0, jax.random.fold_in(own_key, 6)
    for dim, blocks in shards:
        draws = jnp.exp(jax.random.uniform(jax.random.fold_in(own, dim), (blocks,), jnp.float32, least / len(shards), top_value / len(shards)))
        loudness = loudness * jnp.repeat(draws, extent[dim] // blocks).reshape([-1 if axis == dim else 1 for axis in range(len(extent))])
    return loudness


def normal_values(own_key, dims, deviation, limit, cuts=(), kind=jnp.bfloat16):
    values = deviation * jax.random.normal(own_key, dims, jnp.float32)
    if cuts:
        values = values * levels(own_key, dims, cuts, -0.22, 0.18)
    return jnp.clip(values, -limit, limit).astype(kind)


def gaussian_with(stream_key, shape, spread, bound, cuts, heavy, held_as=jnp.bfloat16):
    values = spread * jax.random.normal(stream_key, shape, jnp.float32)
    if cuts:
        values = values * levels(stream_key, shape, cuts, -0.22, 0.18)
    return jnp.clip(strengthened(values, jax.random.fold_in(stream_key, 3), *heavy), -bound, bound).astype(held_as)


def setup_inputs(seed: int = 0) -> dict:
    key_list = jax.random.split(jax.random.key(seed), 7)
    block_input = gaussian_with(key_list[0], (TOKENS, D), 1.0, 8.0, ((0, 8),), (0, 1, 8, 2.0))
    queries = normal_values(key_list[1], (TOKENS, HEADS * DK), 1.0, 6.0, ((0, 8), (1, 4)))
    keys = normal_values(key_list[2], (TOKENS, HEADS * DK), 1.0, 6.0, ((0, 8), (1, 4)))
    w_value = normal_values(key_list[3], (D, HEADS * DV), D ** -0.5, 0.125, ((1, 4),))
    log_decay = draw_log_decay(jax.random.fold_in(key_list[6], 71), 0)
    d_out = normal_values(key_list[5], (TOKENS, HEADS * DV), (TOKENS ** -0.5), 0.125, ((0, 8), (1, 4)))
    return dict(block_input=block_input, queries=queries, keys=keys, w_value=w_value, log_decay=log_decay, d_out=d_out)


def split_heads(array, block_len, width):
    length = array.shape[0]
    return array.reshape(length // block_len, block_len, -1, width).transpose(2, 0, 1, 3)


def merge_heads(array):
    return array.transpose(1, 2, 0, 3).reshape(array.shape[1] * array.shape[2], -1)


def product(form, left, right):
    return jnp.einsum(form, left.astype(jnp.float32), right.astype(jnp.float32), precision=lax.Precision.HIGHEST)


def reference(block_input, queries, keys, w_value, log_decay, d_out):
    q_scale = DK ** -0.5
    values = jnp.dot(block_input, w_value, preferred_element_type=jnp.float32).astype(jnp.bfloat16)
    block_len = 32
    q_heads = split_heads(queries, block_len, DK).astype(jnp.float32) * q_scale
    k_heads = split_heads(keys, block_len, DK).astype(jnp.float32)
    v_heads = split_heads(values, block_len, DV)
    g_heads = split_heads(log_decay, block_len, DK).astype(jnp.float32)
    o_grad = split_heads(d_out, block_len, DV)
    cumlog = jnp.cumsum(g_heads, axis=2)
    last_log = cumlog[:, :, -1:, :]
    k_tail = jnp.exp(last_log - cumlog)
    q_grown = (q_heads * jnp.exp(cumlog)).astype(jnp.bfloat16)
    k_shrunk = (k_heads * jnp.exp(-cumlog)).astype(jnp.bfloat16)
    k_tailed = (k_heads * k_tail).astype(jnp.bfloat16)
    causal = jnp.tril(jnp.ones((block_len, block_len), jnp.float32))
    out_dots = (product('hbcv,hbsv->hbcs', o_grad, v_heads) * causal).astype(jnp.bfloat16)
    key_dots = (product('hbcd,hbsd->hbcs', q_grown, k_shrunk) * causal).astype(jnp.bfloat16)
    increments = product('hbcd,hbcv->hbdv', k_tailed, v_heads)
    backwards = product('hbcd,hbcv->hbdv', q_grown, o_grad)
    block_decay = jnp.exp(last_log[:, :, 0, :])

    def leading(array):
        return jnp.moveaxis(array, 1, 0)

    def forward_step(carried, inputs):
        decay_block, grown = inputs
        return decay_block[:, :, None] * carried + grown, carried

    zero_state = jnp.zeros((HEADS, DK, DV), jnp.float32)
    _, entering = lax.scan(forward_step, zero_state, (leading(block_decay), leading(increments)))

    def backward_step(adjoint, inputs):
        decay_block, grown = inputs
        return grown + decay_block[:, :, None] * adjoint, adjoint

    _, from_right = lax.scan(backward_step, zero_state, (leading(block_decay), leading(backwards)), reverse=True)
    entering = jnp.moveaxis(entering, 0, 1)
    from_right = jnp.moveaxis(from_right, 0, 1)
    q_adjoint = jnp.exp(cumlog) * (product('hbcv,hbdv->hbcd', o_grad, entering) + product('hbcs,hbsd->hbcd', out_dots, k_shrunk))
    k_grad = jnp.exp(-cumlog) * product('hbcs,hbcd->hbsd', out_dots, q_grown) + k_tail * product('hbsv,hbdv->hbsd', v_heads, from_right)
    v_grad = product('hbcs,hbcv->hbsv', key_dots, o_grad) + product('hbsd,hbdv->hbsv', k_tailed, from_right)
    decay_terms = merge_heads(q_heads * q_adjoint - k_heads * k_grad)
    d_log_decay = jnp.flip(jnp.cumsum(jnp.flip(decay_terms, 0), 0), 0)
    value_grad = merge_heads(v_grad).astype(jnp.bfloat16)
    d_w_value = lax.dot_general(block_input, value_grad, (((0,), (0,)), ((), ())), preferred_element_type=jnp.float32)
    row_norms = jnp.sum(d_w_value * d_w_value, axis=1)
    return (merge_heads(q_adjoint * q_scale).astype(jnp.bfloat16), merge_heads(k_grad).astype(jnp.bfloat16), d_log_decay, d_w_value, row_norms)
```

```python
import functools

import jax
import jax.numpy as jnp
from jax import lax
from jax.experimental import pallas as pl
from jax.experimental.pallas import tpu as pltpu
from jax.sharding import PartitionSpec as P

DK = 128
DV = 256
BLOCK = 32
F32 = jnp.float32
BF16 = jnp.bfloat16
MESH = pl.DeviceIdType.MESH


def nn(left, right):
    return lax.dot_general(left, right, (((1,), (0,)), ((), ())), preferred_element_type=F32)


def nt(left, right):
    return lax.dot_general(left, right, (((1,), (1,)), ((), ())), preferred_element_type=F32)


def tn(left, right):
    return lax.dot_general(left, right, (((0,), (0,)), ((), ())), preferred_element_type=F32)


def pieces(value, count):
    parts = []
    for _ in range(count):
        part = value.astype(BF16)
        parts.append(part)
        value = value - part.astype(F32)
    return parts


def ring_place(z, x, nz, nx):
    r = nz - 1 - z
    across = jnp.where(r % 2 == 0, x - 1, nx - 1 - x)
    return jnp.where(x == 0, z, nz + r * (nx - 1) + across)


def ring_member(p, nz, nx):
    u = jnp.maximum(p - nz, 0)
    r = u // (nx - 1)
    w = u % (nx - 1)
    x = jnp.where(r % 2 == 0, 1 + w, nx - 1 - w)
    return jnp.where(p < nz, p * nx, (nz - 1 - r) * nx + x)


def kernel(
    n, nx, ntp,
    x_ref, q_ref, k_ref, w_ref, g_ref, o_ref,
    dq_ref, dk_ref, dg_ref, dw_ref, rn_ref,
    c_buf, span_buf, v_buf, qg_buf, kt_buf, ks_buf, y_buf, kp_buf, vp_buf, st_buf, xt_buf, vg_buf,
    a_out, a_in, z_out, z_in, z_acc, c_out, c_in, first, part, ring, norm_out, norm_in,
    a_send, a_recv, z_send, z_recv, c_send, c_recv, r_send, r_recv, n_send, n_recv,
):
    nz = n // nx
    me = lax.axis_index("sp")
    mine = lax.axis_index("tp")
    z, x = me // nx, me % nx
    tokens, heads = q_ref.shape[0], q_ref.shape[1] // DK
    blocks = tokens // BLOCK
    dvx = DV // nx
    scale = DK ** (-0.5)
    barrier = pltpu.get_barrier_semaphore()
    for off in range(1, n):
        pl.semaphore_signal(barrier, inc=1, device_id={"sp": (me + off) % n}, device_id_type=MESH)
    for off in range(1, ntp):
        pl.semaphore_signal(barrier, inc=1, device_id={"tp": (mine + off) % ntp}, device_id_type=MESH)

    row = lax.broadcasted_iota(jnp.int32, (tokens, tokens), 0)
    col = lax.broadcasted_iota(jnp.int32, (tokens, tokens), 1)
    below = col <= row
    inside = below & (col // BLOCK == row // BLOCK)
    tri = jnp.where(below, 1.0, 0.0).astype(BF16)
    tri_in = jnp.where(inside, 1.0, 0.0).astype(BF16)
    upper = jnp.where(col >= row, 1.0, 0.0).astype(BF16)
    last_in = jnp.where(col // BLOCK == row // BLOCK, 1.0, 0.0).astype(BF16)

    def hd(h):
        return slice(h * DK, (h + 1) * DK)

    def hv(h):
        return slice(h * DV, (h + 1) * DV)

    g_parts = pieces(g_ref[...], 3)
    span_buf[...] = sum(nn(tri, part_) for part_ in g_parts)
    c_buf[...] = sum(nn(tri_in, part_) for part_ in g_parts)
    total = span_buf[tokens - 1 : tokens, :]
    decay = jnp.exp(total)

    def scatter_copy(d, m):
        return pltpu.make_async_remote_copy(
            src_ref=a_out.at[d, m], dst_ref=a_in.at[d, x],
            send_sem=a_send.at[d, m], recv_sem=a_recv.at[d, x],
            device_id={"sp": z * nx + m}, device_id_type=MESH)

    def scatter_wait(d, m):
        pltpu.make_async_remote_copy(
            src_ref=a_out.at[d, m], dst_ref=a_in.at[d, m],
            send_sem=a_send.at[d, m], recv_sem=a_recv.at[d, m],
            device_id={"sp": z * nx + m}, device_id_type=MESH).wait_recv()

    def give(d, totals):
        for m in range(nx):
            for h in range(heads):
                a_out[d, m, h, :dvx, :] = totals[h][m * dvx : (m + 1) * dvx]
                a_out[d, m, h, dvx:, :] = jnp.broadcast_to(decay[:, hd(h)], (8, DK))
        for m in range(nx):
            @pl.when(m != x)
            def _():
                scatter_copy(d, m).start()

            @pl.when(m == x)
            def _():
                a_in[d, m] = a_out[d, m]

    q_all = q_ref[...].astype(F32) * scale
    q_span = (q_all * jnp.exp(span_buf[...])).astype(BF16)
    adjoints = [tn(o_ref[:, hv(h)], q_span[:, hd(h)]) for h in range(heads)]
    pl.semaphore_wait(barrier, n - 1 + ntp - 1)
    give(1, adjoints)

    for h in range(heads):
        v_buf[:, hv(h)] = nn(x_ref[...], w_ref[:, hv(h)]).astype(BF16)
    k_all = k_ref[...].astype(F32)
    k_far = jnp.exp(total - span_buf[...])
    k_span = (k_all * k_far).astype(BF16)
    states = [tn(v_buf[:, hv(h)], k_span[:, hd(h)]) for h in range(heads)]
    give(0, states)

    def plane(target):
        return {"sp": target * nx + x}

    def order(d):
        return range(nx) if d == 0 else range(nx - 1, -1, -1)

    def plane_copy(d, dz):
        return pltpu.make_async_remote_copy(
            src_ref=z_out.at[d], dst_ref=z_in.at[d, z],
            send_sem=z_send.at[d, dz], recv_sem=z_recv.at[d, z],
            device_id=plane(z + dz if d == 0 else z - dz), device_id_type=MESH)

    def plane_there(d, dz):
        return z + dz < nz if d == 0 else z - dz >= 0

    def combine(d):
        for m in range(nx):
            @pl.when(m != x)
            def _():
                scatter_wait(d, m)
        for h in range(heads):
            acc, dec = None, None
            for m in order(d):
                local, rate = a_in[d, m, h, :dvx, :], a_in[d, m, h, dvx:, :]
                acc = local if acc is None else local + rate[:1] * acc
                dec = rate if dec is None else rate * dec
            z_out[d, h, :dvx, :] = acc
            z_out[d, h, dvx:, :] = dec
        for dz in range(1, nz):
            @pl.when(plane_there(d, dz))
            def _():
                plane_copy(d, dz).start()

    combine(1)
    combine(0)

    cum = c_buf[...]
    block_end = sum(nn(last_in, part_) for part_ in g_parts)
    k_tail = jnp.exp(block_end - cum)
    grow = jnp.exp(cum)
    qg_buf[...] = (q_all * grow).astype(BF16)
    ks_buf[...] = (k_all * jnp.exp(-cum)).astype(BF16)
    kt_buf[...] = (k_all * k_tail).astype(BF16)
    st_buf[...] = jnp.zeros_like(st_buf)

    def span_step(step, carry):
        at = pl.multiple_of(step * BLOCK, BLOCK)
        back = pl.multiple_of((blocks - 1 - step) * BLOCK, BLOCK)
        rows, rows_b = pl.ds(at, BLOCK), pl.ds(back, BLOCK)
        for h in range(heads):
            keep = jnp.exp(c_buf[rows, hd(h)][BLOCK - 1 :])
            state = st_buf[0, h]
            y_buf[rows, hd(h)] = nn(o_ref[rows, hv(h)], state.astype(BF16))
            st_buf[0, h] = keep * state + tn(v_buf[rows, hv(h)], kt_buf[rows, hd(h)])
            keep = jnp.exp(c_buf[rows_b, hd(h)][BLOCK - 1 :])
            adjoint = st_buf[1, h]
            narrow = adjoint.astype(BF16)
            kp_buf[rows_b, hd(h)] = nn(v_buf[rows_b, hv(h)], narrow)
            vp_buf[rows_b, hv(h)] = nt(kt_buf[rows_b, hd(h)], narrow)
            st_buf[1, h] = keep * adjoint + tn(o_ref[rows_b, hv(h)], qg_buf[rows_b, hd(h)])
        return carry

    lax.fori_loop(0, blocks, span_step, 0)

    for h in range(heads):
        dots = jnp.where(inside, nt(o_ref[:, hv(h)], v_buf[:, hv(h)]), 0.0).astype(BF16)
        y_buf[:, hd(h)] += nn(dots, ks_buf[:, hd(h)])
        kp_buf[:, hd(h)] = (
            k_tail[:, hd(h)] * kp_buf[:, hd(h)]
            + jnp.exp(-cum[:, hd(h)]) * tn(dots, qg_buf[:, hd(h)])
        )
        dots = jnp.where(inside, nt(qg_buf[:, hd(h)], ks_buf[:, hd(h)]), 0.0).astype(BF16)
        vp_buf[:, hv(h)] += tn(dots, o_ref[:, hv(h)])

    depth = x_ref.shape[1]
    for at in range(0, depth, 256):
        xt_buf[at : at + 256, :] = x_ref[:, at : at + 256].T

    def member_copy(d, m):
        return pltpu.make_async_remote_copy(
            src_ref=c_out.at[d, m], dst_ref=c_in.at[d, x],
            send_sem=c_send.at[d, m], recv_sem=c_recv.at[d, x],
            device_id={"sp": z * nx + m}, device_id_type=MESH)

    def spread(d):
        z_acc[...] = jnp.zeros_like(z_acc)
        for zp in (range(nz) if d == 0 else range(nz - 1, -1, -1)):
            @pl.when(zp < z if d == 0 else zp > z)
            def _():
                pltpu.make_async_remote_copy(
                    src_ref=z_out.at[d], dst_ref=z_in.at[d, zp],
                    send_sem=z_send.at[d, 0], recv_sem=z_recv.at[d, zp],
                    device_id=plane(zp), device_id_type=MESH).wait_recv()
                for h in range(heads):
                    z_acc[h] = z_in[d, zp, h, :dvx, :] + z_in[d, zp, h, dvx : dvx + 1, :] * z_acc[h]
        for h in range(heads):
            acc = z_acc[h]
            for m in order(d):
                c_out[d, m, h] = acc
                acc = a_in[d, m, h, :dvx, :] + a_in[d, m, h, dvx : dvx + 1, :] * acc
        for m in range(nx):
            @pl.when(m != x)
            def _():
                member_copy(d, m).start()

            @pl.when(m == x)
            def _():
                c_in[d, m] = c_out[d, m]

    def entering(d):
        for m in range(nx):
            @pl.when(m != x)
            def _():
                pltpu.make_async_remote_copy(
                    src_ref=c_out.at[d, m], dst_ref=c_in.at[d, m],
                    send_sem=c_send.at[d, m], recv_sem=c_recv.at[d, m],
                    device_id={"sp": z * nx + m}, device_id_type=MESH).wait_recv()
        return [
            jnp.concatenate([c_in[d, m, h] for m in range(nx)], axis=0) for h in range(heads)
        ]

    spread(1)
    spread(0)
    from_right = entering(1)
    for h in range(heads):
        narrow = from_right[h].astype(BF16)
        vg_buf[:, hv(h)] = (vp_buf[:, hv(h)] + nt(k_span[:, hd(h)], narrow)).astype(BF16)

    own = dw_ref.shape[0]
    half_r, half_c = own // 2, dw_ref.shape[1] // 2
    p = ring_place(z, x, nz, nx)
    ahead = ring_member((p + 1) % n, nz, nx)
    behind = ring_member((p + n - 1) % n, nz, nx)

    def share(d, u, owner):
        rows_ = pl.ds(pl.multiple_of(owner * own + u * half_r, half_r), half_r)
        return nn(xt_buf[rows_, :], vg_buf[:, d * half_c : (d + 1) * half_c])

    def ring_copy(step, d, u, src):
        return pltpu.make_async_remote_copy(
            src_ref=src, dst_ref=ring.at[step, d, u],
            send_sem=r_send.at[step, d, u], recv_sem=r_recv.at[step, d, u],
            device_id={"sp": ahead if d == 0 else behind}, device_id_type=MESH)

    def owner_at(step, d):
        return ring_member((p + n - step - 1) % n if d == 0 else (p + step + 1) % n, nz, nx)

    for u in range(2):
        for d in range(2):
            first[d, u] = share(d, u, owner_at(0, d))
            ring_copy(0, d, u, first.at[d, u]).start()

    state_in = entering(0)
    for h in range(heads):
        k_grad = kp_buf[:, hd(h)] + k_far[:, hd(h)] * nn(v_buf[:, hv(h)], from_right[h].astype(BF16))
        dk_ref[:, hd(h)] = k_grad.astype(BF16)
        q_grad = grow[:, hd(h)] * y_buf[:, hd(h)] + jnp.exp(span_buf[:, hd(h)]) * nn(
            o_ref[:, hv(h)], state_in[h].astype(BF16)
        )
        dq_ref[:, hd(h)] = (q_grad * scale).astype(BF16)
        terms = q_all[:, hd(h)] * q_grad - k_all[:, hd(h)] * k_grad
        span_end = st_buf[0, h] + decay[:, hd(h)] * state_in[h]
        carry = jnp.sum(from_right[h] * span_end, axis=0, keepdims=True)
        dg_ref[:, hd(h)] = sum(nn(upper, part_) for part_ in pieces(terms, 3)) + carry

    def ring_step(step, carry):
        for d in range(2):
            for u in range(2):
                part[d, u] = share(d, u, owner_at(step, d))
        for u in range(2):
            for d in range(2):
                ring_copy(step - 1, d, u, first.at[d, u]).wait_recv()
                ring[step - 1, d, u] += part[d, u]
                ring_copy(step, d, u, ring.at[step - 1, d, u]).start()
        return carry

    lax.fori_loop(1, n - 1, ring_step, 0)

    for d in range(2):
        for u in range(2):
            part[d, u] = share(d, u, me)
    for u in range(2):
        squares = 0.0
        for d in range(2):
            ring_copy(n - 2, d, u, first.at[d, u]).wait_recv()
            done = ring[n - 2, d, u] + part[d, u]
            dw_ref[u * half_r : (u + 1) * half_r, d * half_c : (d + 1) * half_c] = done
            for at in range(0, half_c, 128):
                squares = squares + done[:, at : at + 128] * done[:, at : at + 128]
        norm_out[u] = jnp.broadcast_to(jnp.sum(squares.T, axis=0, keepdims=True), (8, half_r))

    def norm_copy(off):
        return pltpu.make_async_remote_copy(
            src_ref=norm_out, dst_ref=norm_in.at[off],
            send_sem=n_send.at[off], recv_sem=n_recv.at[off],
            device_id={"tp": (mine + off) % ntp}, device_id_type=MESH)

    for off in range(1, ntp):
        norm_copy(off).start()

    for d in range(2):
        for m in range(nx):
            @pl.when(m != x)
            def _():
                scatter_copy(d, m).wait_send()
                member_copy(d, m).wait_send()
        for dz in range(1, nz):
            @pl.when(plane_there(d, dz))
            def _():
                plane_copy(d, dz).wait_send()

    def sent(step, carry):
        for u in range(2):
            for d in range(2):
                ring_copy(step, d, u, first.at[d, u]).wait_send()
        return carry

    lax.fori_loop(0, n - 1, sent, 0)
    norms = norm_out[...]
    for off in range(1, ntp):
        norm_copy(off).wait()
        norms = norms + norm_in[off]
    rn_ref[...] = norms


def on_device(n, nx, ntp, block_input, queries, keys, w_value, log_decay, d_out):
    tokens, wide = queries.shape
    heads = wide // DK
    cols = w_value.shape[1]
    depth = block_input.shape[1]
    own = depth // n
    nz = n // nx
    dvx = DV // nx
    vm = pltpu.VMEM
    dma = pltpu.SemaphoreType.DMA
    out = pl.pallas_call(
        functools.partial(kernel, n, nx, ntp),
        out_shape=(
            jax.ShapeDtypeStruct((tokens, wide), BF16),
            jax.ShapeDtypeStruct((tokens, wide), BF16),
            jax.ShapeDtypeStruct((tokens, wide), F32),
            jax.ShapeDtypeStruct((own, cols), F32),
            jax.ShapeDtypeStruct((2, 8, own // 2), F32),
        ),
        in_specs=[pl.BlockSpec(memory_space=vm)] * 6,
        out_specs=(pl.BlockSpec(memory_space=vm),) * 5,
        scratch_shapes=[
            vm((tokens, wide), F32),
            vm((tokens, wide), F32),
            vm((tokens, cols), BF16),
            vm((tokens, wide), BF16),
            vm((tokens, wide), BF16),
            vm((tokens, wide), BF16),
            vm((tokens, wide), F32),
            vm((tokens, wide), F32),
            vm((tokens, cols), F32),
            vm((2, heads, DV, DK), F32),
            vm((depth, tokens), BF16),
            vm((tokens, cols), BF16),
            vm((2, nx, heads, dvx + 8, DK), F32),
            vm((2, nx, heads, dvx + 8, DK), F32),
            vm((2, heads, dvx + 8, DK), F32),
            vm((2, nz, heads, dvx + 8, DK), F32),
            vm((heads, dvx, DK), F32),
            vm((2, nx, heads, dvx, DK), F32),
            vm((2, nx, heads, dvx, DK), F32),
            vm((2, 2, own // 2, cols // 2), F32),
            vm((2, 2, own // 2, cols // 2), F32),
            vm((n - 1, 2, 2, own // 2, cols // 2), F32),
            vm((2, 8, own // 2), F32),
            vm((ntp, 2, 8, own // 2), F32),
            dma((2, nx)),
            dma((2, nx)),
            dma((2, nz)),
            dma((2, nz)),
            dma((2, nx)),
            dma((2, nx)),
            dma((n - 1, 2, 2)),
            dma((n - 1, 2, 2)),
            dma((ntp,)),
            dma((ntp,)),
        ],
        compiler_params=pltpu.CompilerParams(
            collective_id=0, has_side_effects=True, vmem_limit_bytes=56 * 1024 * 1024
        ),
    )(block_input, queries, keys, w_value, log_decay, d_out)
    return (*out[:4], out[4][:, 0].reshape(-1))


def solution(mesh):
    n, ntp = mesh.shape["sp"], mesh.shape["tp"]
    nx = 1 << ((n.bit_length() - 1) // 2)
    placed = (
        P("sp", None),
        P("sp", "tp"),
        P("sp", "tp"),
        P(None, "tp"),
        P("sp", "tp"),
        P("sp", "tp"),
    )
    return jax.shard_map(
        functools.partial(on_device, n, nx, ntp),
        mesh=mesh,
        in_specs=placed,
        out_specs=(P("sp", "tp"), P("sp", "tp"), P("sp", "tp"), P("sp", "tp"), P("sp")),
        check_vma=False,
    )
```

```python
import functools

import jax
import jax.numpy as jnp
from jax import lax
from jax.experimental import pallas as pl
from jax.experimental.pallas import tpu as pltpu
from jax.sharding import PartitionSpec as P

DK = 128
DV = 256
BLOCK = 32
F32 = jnp.float32
BF16 = jnp.bfloat16
MESH = pl.DeviceIdType.MESH


def nn(left, right):
    return lax.dot_general(left, right, (((1,), (0,)), ((), ())), preferred_element_type=F32)


def nt(left, right):
    return lax.dot_general(left, right, (((1,), (1,)), ((), ())), preferred_element_type=F32)


def tn(left, right):
    return lax.dot_general(left, right, (((0,), (0,)), ((), ())), preferred_element_type=F32)


def pieces(value, count):
    parts = []
    for _ in range(count):
        part = value.astype(BF16)
        parts.append(part)
        value = value - part.astype(F32)
    return parts


def ring_place(z, x, nz, nx):
    r = nz - 1 - z
    across = jnp.where(r % 2 == 0, x - 1, nx - 1 - x)
    return jnp.where(x == 0, z, nz + r * (nx - 1) + across)


def ring_member(p, nz, nx):
    u = jnp.maximum(p - nz, 0)
    r = u // (nx - 1)
    w = u % (nx - 1)
    x = jnp.where(r % 2 == 0, 1 + w, nx - 1 - w)
    return jnp.where(p < nz, p * nx, (nz - 1 - r) * nx + x)


def kernel(
    n, nx, ntp,
    x_ref, q_ref, k_ref, w_ref, g_ref, o_ref,
    dq_ref, dk_ref, dg_ref, dw_ref, rn_ref,
    c_buf, span_buf, v_buf, qg_buf, kt_buf, ks_buf, y_buf, kp_buf, vp_buf, st_buf, xt_buf, vg_buf,
    a_out, a_in, z_out, z_in, z_acc, c_out, c_in, first, part, ring, norm_out, norm_in,
    a_send, a_recv, z_send, z_recv, c_send, c_recv, r_send, r_recv, n_send, n_recv,
):
    nz = n // nx
    me = lax.axis_index("sp")
    mine = lax.axis_index("tp")
    z, x = me // nx, me % nx
    tokens, heads = q_ref.shape[0], q_ref.shape[1] // DK
    blocks = tokens // BLOCK
    dvx = DV // nx
    scale = DK ** (-0.5)
    barrier = pltpu.get_barrier_semaphore()
    for off in range(1, n):
        pl.semaphore_signal(barrier, inc=1, device_id={"sp": (me + off) % n}, device_id_type=MESH)
    for off in range(1, ntp):
        pl.semaphore_signal(barrier, inc=1, device_id={"tp": (mine + off) % ntp}, device_id_type=MESH)

    row = lax.broadcasted_iota(jnp.int32, (tokens, tokens), 0)
    col = lax.broadcasted_iota(jnp.int32, (tokens, tokens), 1)
    below = col <= row
    inside = below & (col // BLOCK == row // BLOCK)
    tri = jnp.where(below, 1.0, 0.0).astype(BF16)
    tri_in = jnp.where(inside, 1.0, 0.0).astype(BF16)
    upper = jnp.where(col >= row, 1.0, 0.0).astype(BF16)
    last_in = jnp.where(col // BLOCK == row // BLOCK, 1.0, 0.0).astype(BF16)

    def hd(h):
        return slice(h * DK, (h + 1) * DK)

    def hv(h):
        return slice(h * DV, (h + 1) * DV)

    g_parts = pieces(g_ref[...], 3)
    span_buf[...] = sum(nn(tri, part_) for part_ in g_parts)
    c_buf[...] = sum(nn(tri_in, part_) for part_ in g_parts)
    total = span_buf[tokens - 1 : tokens, :]
    decay = jnp.exp(total)

    def scatter_copy(d, m):
        return pltpu.make_async_remote_copy(
            src_ref=a_out.at[d, m], dst_ref=a_in.at[d, x],
            send_sem=a_send.at[d, m], recv_sem=a_recv.at[d, x],
            device_id={"sp": z * nx + m}, device_id_type=MESH)

    def scatter_wait(d, m):
        pltpu.make_async_remote_copy(
            src_ref=a_out.at[d, m], dst_ref=a_in.at[d, m],
            send_sem=a_send.at[d, m], recv_sem=a_recv.at[d, m],
            device_id={"sp": z * nx + m}, device_id_type=MESH).wait_recv()

    def give(d, totals):
        for m in range(nx):
            for h in range(heads):
                a_out[d, m, h, :dvx, :] = totals[h][m * dvx : (m + 1) * dvx]
                a_out[d, m, h, dvx:, :] = jnp.broadcast_to(decay[:, hd(h)], (8, DK))
        for m in range(nx):
            @pl.when(m != x)
            def _():
                scatter_copy(d, m).start()

            @pl.when(m == x)
            def _():
                a_in[d, m] = a_out[d, m]

    q_all = q_ref[...].astype(F32) * scale
    q_span = (q_all * jnp.exp(span_buf[...])).astype(BF16)
    adjoints = [tn(o_ref[:, hv(h)], q_span[:, hd(h)]) for h in range(heads)]
    pl.semaphore_wait(barrier, n - 1 + ntp - 1)
    give(1, adjoints)

    for h in range(heads):
        v_buf[:, hv(h)] = nn(x_ref[...], w_ref[:, hv(h)]).astype(BF16)
    k_all = k_ref[...].astype(F32)
    k_far = jnp.exp(total - span_buf[...])
    k_span = (k_all * k_far).astype(BF16)
    states = [tn(v_buf[:, hv(h)], k_span[:, hd(h)]) for h in range(heads)]
    give(0, states)

    def plane(target):
        return {"sp": target * nx + x}

    def order(d):
        return range(nx) if d == 0 else range(nx - 1, -1, -1)

    def plane_copy(d, dz):
        return pltpu.make_async_remote_copy(
            src_ref=z_out.at[d], dst_ref=z_in.at[d, z],
            send_sem=z_send.at[d, dz], recv_sem=z_recv.at[d, z],
            device_id=plane(z + dz if d == 0 else z - dz), device_id_type=MESH)

    def plane_there(d, dz):
        return z + dz < nz if d == 0 else z - dz >= 0

    def combine(d):
        for m in range(nx):
            @pl.when(m != x)
            def _():
                scatter_wait(d, m)
        for h in range(heads):
            acc, dec = None, None
            for m in order(d):
                local, rate = a_in[d, m, h, :dvx, :], a_in[d, m, h, dvx:, :]
                acc = local if acc is None else local + rate[:1] * acc
                dec = rate if dec is None else rate * dec
            z_out[d, h, :dvx, :] = acc
            z_out[d, h, dvx:, :] = dec
        for dz in range(1, nz):
            @pl.when(plane_there(d, dz))
            def _():
                plane_copy(d, dz).start()

    combine(1)
    combine(0)

    cum = c_buf[...]
    block_end = sum(nn(last_in, part_) for part_ in g_parts)
    k_tail = jnp.exp(block_end - cum)
    grow = jnp.exp(cum)
    qg_buf[...] = (q_all * grow).astype(BF16)
    ks_buf[...] = (k_all * jnp.exp(-cum)).astype(BF16)
    kt_buf[...] = (k_all * k_tail).astype(BF16)
    st_buf[...] = jnp.zeros_like(st_buf)

    def span_step(step, carry):
        at = pl.multiple_of(step * BLOCK, BLOCK)
        back = pl.multiple_of((blocks - 1 - step) * BLOCK, BLOCK)
        rows, rows_b = pl.ds(at, BLOCK), pl.ds(back, BLOCK)
        for h in range(heads):
            keep = jnp.exp(c_buf[rows, hd(h)][BLOCK - 1 :])
            state = st_buf[0, h]
            y_buf[rows, hd(h)] = nn(o_ref[rows, hv(h)], state.astype(BF16))
            st_buf[0, h] = keep * state + tn(v_buf[rows, hv(h)], kt_buf[rows, hd(h)])
            keep = jnp.exp(c_buf[rows_b, hd(h)][BLOCK - 1 :])
            adjoint = st_buf[1, h]
            narrow = adjoint.astype(BF16)
            kp_buf[rows_b, hd(h)] = nn(v_buf[rows_b, hv(h)], narrow)
            vp_buf[rows_b, hv(h)] = nt(kt_buf[rows_b, hd(h)], narrow)
            st_buf[1, h] = keep * adjoint + tn(o_ref[rows_b, hv(h)], qg_buf[rows_b, hd(h)])
        return carry

    lax.fori_loop(0, blocks, span_step, 0)

    for h in range(heads):
        dots = jnp.where(inside, nt(o_ref[:, hv(h)], v_buf[:, hv(h)]), 0.0).astype(BF16)
        y_buf[:, hd(h)] += nn(dots, ks_buf[:, hd(h)])
        kp_buf[:, hd(h)] = (
            k_tail[:, hd(h)] * kp_buf[:, hd(h)]
            + jnp.exp(-cum[:, hd(h)]) * tn(dots, qg_buf[:, hd(h)])
        )
        dots = jnp.where(inside, nt(qg_buf[:, hd(h)], ks_buf[:, hd(h)]), 0.0).astype(BF16)
        vp_buf[:, hv(h)] += tn(dots, o_ref[:, hv(h)])

    depth = x_ref.shape[1]
    for at in range(0, depth, 256):
        xt_buf[at : at + 256, :] = x_ref[:, at : at + 256].T

    def member_copy(d, m):
        return pltpu.make_async_remote_copy(
            src_ref=c_out.at[d, m], dst_ref=c_in.at[d, x],
            send_sem=c_send.at[d, m], recv_sem=c_recv.at[d, x],
            device_id={"sp": z * nx + m}, device_id_type=MESH)

    def spread(d):
        z_acc[...] = jnp.zeros_like(z_acc)
        for zp in (range(nz) if d == 0 else range(nz - 1, -1, -1)):
            @pl.when(zp < z if d == 0 else zp > z)
            def _():
                pltpu.make_async_remote_copy(
                    src_ref=z_out.at[d], dst_ref=z_in.at[d, zp],
                    send_sem=z_send.at[d, 0], recv_sem=z_recv.at[d, zp],
                    device_id=plane(zp), device_id_type=MESH).wait_recv()
                for h in range(heads):
                    z_acc[h] = z_in[d, zp, h, :dvx, :] + z_in[d, zp, h, dvx : dvx + 1, :] * z_acc[h]
        for h in range(heads):
            acc = z_acc[h]
            for m in order(d):
                c_out[d, m, h] = acc
                acc = a_in[d, m, h, :dvx, :] + a_in[d, m, h, dvx : dvx + 1, :] * acc
        for m in range(nx):
            @pl.when(m != x)
            def _():
                member_copy(d, m).start()

            @pl.when(m == x)
            def _():
                c_in[d, m] = c_out[d, m]

    def entering(d):
        for m in range(nx):
            @pl.when(m != x)
            def _():
                pltpu.make_async_remote_copy(
                    src_ref=c_out.at[d, m], dst_ref=c_in.at[d, m],
                    send_sem=c_send.at[d, m], recv_sem=c_recv.at[d, m],
                    device_id={"sp": z * nx + m}, device_id_type=MESH).wait_recv()
        return [
            jnp.concatenate([c_in[d, m, h] for m in range(nx)], axis=0) for h in range(heads)
        ]

    spread(1)
    spread(0)
    from_right = entering(1)
    for h in range(heads):
        narrow = from_right[h].astype(BF16)
        vg_buf[:, hv(h)] = (vp_buf[:, hv(h)] + nt(k_span[:, hd(h)], narrow)).astype(BF16)

    own = dw_ref.shape[0]
    half_r, half_c = own // 2, dw_ref.shape[1] // 2
    p = ring_place(z, x, nz, nx)
    ahead = ring_member((p + 1) % n, nz, nx)
    behind = ring_member((p + n - 1) % n, nz, nx)

    def share(d, u, owner):
        rows_ = pl.ds(pl.multiple_of(owner * own + u * half_r, half_r), half_r)
        return nn(xt_buf[rows_, :], vg_buf[:, d * half_c : (d + 1) * half_c])

    def ring_copy(step, d, u, src):
        return pltpu.make_async_remote_copy(
            src_ref=src, dst_ref=ring.at[step, d, u],
            send_sem=r_send.at[step, d, u], recv_sem=r_recv.at[step, d, u],
            device_id={"sp": ahead if d == 0 else behind}, device_id_type=MESH)

    def owner_at(step, d):
        return ring_member((p + n - step - 1) % n if d == 0 else (p + step + 1) % n, nz, nx)

    for u in range(2):
        for d in range(2):
            first[d, u] = share(d, u, owner_at(0, d))
            ring_copy(0, d, u, first.at[d, u]).start()

    state_in = entering(0)
    for h in range(heads):
        k_grad = kp_buf[:, hd(h)] + k_far[:, hd(h)] * nn(v_buf[:, hv(h)], from_right[h].astype(BF16))
        dk_ref[:, hd(h)] = k_grad.astype(BF16)
        q_grad = grow[:, hd(h)] * y_buf[:, hd(h)] + jnp.exp(span_buf[:, hd(h)]) * nn(
            o_ref[:, hv(h)], state_in[h].astype(BF16)
        )
        dq_ref[:, hd(h)] = (q_grad * scale).astype(BF16)
        terms = q_all[:, hd(h)] * q_grad - k_all[:, hd(h)] * k_grad
        span_end = st_buf[0, h] + decay[:, hd(h)] * state_in[h]
        carry = jnp.sum(from_right[h] * span_end, axis=0, keepdims=True)
        dg_ref[:, hd(h)] = sum(nn(upper, part_) for part_ in pieces(terms, 3)) + carry

    def ring_step(step, carry):
        for d in range(2):
            for u in range(2):
                part[d, u] = share(d, u, owner_at(step, d))
        for u in range(2):
            for d in range(2):
                ring_copy(step - 1, d, u, first.at[d, u]).wait_recv()
                ring[step - 1, d, u] += part[d, u]
                ring_copy(step, d, u, ring.at[step - 1, d, u]).start()
        return carry

    lax.fori_loop(1, n - 1, ring_step, 0)

    for d in range(2):
        for u in range(2):
            part[d, u] = share(d, u, me)
    for u in range(2):
        squares = 0.0
        for d in range(2):
            ring_copy(n - 2, d, u, first.at[d, u]).wait_recv()
            done = ring[n - 2, d, u] + part[d, u]
            dw_ref[u * half_r : (u + 1) * half_r, d * half_c : (d + 1) * half_c] = done
            for at in range(0, half_c, 128):
                squares = squares + done[:, at : at + 128] * done[:, at : at + 128]
        norm_out[u] = jnp.broadcast_to(jnp.sum(squares.T, axis=0, keepdims=True), (8, half_r))

    def norm_copy(off):
        return pltpu.make_async_remote_copy(
            src_ref=norm_out, dst_ref=norm_in.at[off],
            send_sem=n_send.at[off], recv_sem=n_recv.at[off],
            device_id={"tp": (mine + off) % ntp}, device_id_type=MESH)

    for off in range(1, ntp):
        norm_copy(off).start()

    for d in range(2):
        for m in range(nx):
            @pl.when(m != x)
            def _():
                scatter_copy(d, m).wait_send()
                member_copy(d, m).wait_send()
        for dz in range(1, nz):
            @pl.when(plane_there(d, dz))
            def _():
                plane_copy(d, dz).wait_send()

    def sent(step, carry):
        for u in range(2):
            for d in range(2):
                ring_copy(step, d, u, first.at[d, u]).wait_send()
        return carry

    lax.fori_loop(0, n - 1, sent, 0)
    norms = norm_out[...]
    for off in range(1, ntp):
        norm_copy(off).wait()
        norms = norms + norm_in[off]
    rn_ref[...] = norms


def finish(*refs):
    for source, target in zip(refs[:4], refs[5:9]):
        target[...] = source[...]
    refs[9][...] = refs[4][:, :1]


def on_device(n, nx, ntp, block_input, queries, keys, w_value, log_decay, d_out):
    tokens, wide = queries.shape
    heads = wide // DK
    cols = w_value.shape[1]
    depth = block_input.shape[1]
    own = depth // n
    nz = n // nx
    dvx = DV // nx
    vm = pltpu.VMEM
    dma = pltpu.SemaphoreType.DMA
    out = pl.pallas_call(
        functools.partial(kernel, n, nx, ntp),
        out_shape=(
            jax.ShapeDtypeStruct((tokens, wide), BF16),
            jax.ShapeDtypeStruct((tokens, wide), BF16),
            jax.ShapeDtypeStruct((tokens, wide), F32),
            jax.ShapeDtypeStruct((own, cols), F32),
            jax.ShapeDtypeStruct((2, 8, own // 2), F32),
        ),
        in_specs=[pl.BlockSpec(memory_space=vm)] * 6,
        out_specs=(pl.BlockSpec(memory_space=vm),) * 5,
        scratch_shapes=[
            vm((tokens, wide), F32),
            vm((tokens, wide), F32),
            vm((tokens, cols), BF16),
            vm((tokens, wide), BF16),
            vm((tokens, wide), BF16),
            vm((tokens, wide), BF16),
            vm((tokens, wide), F32),
            vm((tokens, wide), F32),
            vm((tokens, cols), F32),
            vm((2, heads, DV, DK), F32),
            vm((depth, tokens), BF16),
            vm((tokens, cols), BF16),
            vm((2, nx, heads, dvx + 8, DK), F32),
            vm((2, nx, heads, dvx + 8, DK), F32),
            vm((2, heads, dvx + 8, DK), F32),
            vm((2, nz, heads, dvx + 8, DK), F32),
            vm((heads, dvx, DK), F32),
            vm((2, nx, heads, dvx, DK), F32),
            vm((2, nx, heads, dvx, DK), F32),
            vm((2, 2, own // 2, cols // 2), F32),
            vm((2, 2, own // 2, cols // 2), F32),
            vm((n - 1, 2, 2, own // 2, cols // 2), F32),
            vm((2, 8, own // 2), F32),
            vm((ntp, 2, 8, own // 2), F32),
            dma((2, nx)),
            dma((2, nx)),
            dma((2, nz)),
            dma((2, nz)),
            dma((2, nx)),
            dma((2, nx)),
            dma((n - 1, 2, 2)),
            dma((n - 1, 2, 2)),
            dma((ntp,)),
            dma((ntp,)),
        ],
        compiler_params=pltpu.CompilerParams(
            collective_id=0, has_side_effects=True, vmem_limit_bytes=32 * 1024 * 1024
        ),
    )(block_input, queries, keys, w_value, log_decay, d_out)
    final = pl.pallas_call(
        finish,
        out_shape=tuple(jax.ShapeDtypeStruct(a.shape, a.dtype) for a in out[:4])
        + (jax.ShapeDtypeStruct((2, 1, own // 2), F32),),
        in_specs=[pl.BlockSpec(memory_space=vm)] * 5,
        out_specs=(pl.BlockSpec(memory_space=vm),) * 5,
        compiler_params=pltpu.CompilerParams(vmem_limit_bytes=8 * 1024 * 1024),
    )(*out)
    return (*final[:4], final[4].reshape(-1))


def solution(mesh):
    n, ntp = mesh.shape["sp"], mesh.shape["tp"]
    nx = 1 << ((n.bit_length() - 1) // 2)
    placed = (
        P("sp", None),
        P("sp", "tp"),
        P("sp", "tp"),
        P(None, "tp"),
        P("sp", "tp"),
        P("sp", "tp"),
    )
    return jax.shard_map(
        functools.partial(on_device, n, nx, ntp),
        mesh=mesh,
        in_specs=placed,
        out_specs=(P("sp", "tp"), P("sp", "tp"), P("sp", "tp"), P("sp", "tp"), P("sp")),
        check_vma=False,
    )
```

```python
import functools

import jax
import jax.numpy as jnp
from jax import lax
from jax.experimental import pallas as pl
from jax.experimental.pallas import tpu as pltpu
from jax.sharding import PartitionSpec as P

DK = 128
DV = 256
BLOCK = 32
F32 = jnp.float32
BF16 = jnp.bfloat16
MESH = pl.DeviceIdType.MESH


def nn(left, right):
    return lax.dot_general(left, right, (((1,), (0,)), ((), ())), preferred_element_type=F32)


def nt(left, right):
    return lax.dot_general(left, right, (((1,), (1,)), ((), ())), preferred_element_type=F32)


def tn(left, right):
    return lax.dot_general(left, right, (((0,), (0,)), ((), ())), preferred_element_type=F32)


def pieces(value, count):
    parts = []
    for _ in range(count):
        part = value.astype(BF16)
        parts.append(part)
        value = value - part.astype(F32)
    return parts


def ring_place(z, x, nz, nx):
    r = nz - 1 - z
    across = jnp.where(r % 2 == 0, x - 1, nx - 1 - x)
    return jnp.where(x == 0, z, nz + r * (nx - 1) + across)


def ring_member(p, nz, nx):
    u = jnp.maximum(p - nz, 0)
    r = u // (nx - 1)
    w = u % (nx - 1)
    x = jnp.where(r % 2 == 0, 1 + w, nx - 1 - w)
    return jnp.where(p < nz, p * nx, (nz - 1 - r) * nx + x)


def kernel(
    n, nx, ntp,
    x_hbm, q_hbm, k_hbm, w_hbm, g_hbm, o_hbm,
    dq_ref, dk_ref, dg_ref, dw_ref, rn_ref,
    x_ref, q_ref, k_ref, w_ref, g_ref, o_ref, in_sem,
    c_buf, span_buf, v_buf, qg_buf, kt_buf, ks_buf, y_buf, kp_buf, vp_buf, st_buf, xt_buf, vg_buf,
    a_out, a_in, z_out, z_in, z_acc, c_out, c_in, h_out, h_in, b_out, b_in, fr_buf,
    first, part, ring, norm_out, norm_in,
    a_send, a_recv, z_send, z_recv, c_send, c_recv, h_send, h_recv, b_send, b_recv, r_send, r_recv, n_send, n_recv,
):
    nz = n // nx
    me = lax.axis_index("sp")
    mine = lax.axis_index("tp")
    z, x = me // nx, me % nx
    tokens, heads = q_ref.shape[0], q_ref.shape[1] // DK
    blocks = tokens // BLOCK
    dvx = DV // nx
    scale = DK ** (-0.5)
    loads = [
        pltpu.make_async_copy(source, target, in_sem.at[i])
        for i, (source, target) in enumerate(
            [(g_hbm, g_ref), (q_hbm, q_ref), (o_hbm, o_ref), (k_hbm, k_ref), (x_hbm, x_ref), (w_hbm, w_ref)]
        )
    ]
    for load in loads:
        load.start()
    barrier = pltpu.get_barrier_semaphore()
    for off in range(1, nx):
        pl.semaphore_signal(
            barrier, inc=1, device_id={"sp": z * nx + (x + off) % nx}, device_id_type=MESH)
    for off in range(1, nz):
        pl.semaphore_signal(
            barrier, inc=1, device_id={"sp": (z + off) % nz * nx + x}, device_id_type=MESH)
    for off in range(1, ntp):
        pl.semaphore_signal(barrier, inc=1, device_id={"tp": (mine + off) % ntp}, device_id_type=MESH)

    row = lax.broadcasted_iota(jnp.int32, (tokens, tokens), 0)
    col = lax.broadcasted_iota(jnp.int32, (tokens, tokens), 1)
    below = col <= row
    inside = below & (col // BLOCK == row // BLOCK)
    tri = jnp.where(below, 1.0, 0.0).astype(BF16)
    tri_in = jnp.where(inside, 1.0, 0.0).astype(BF16)
    upper = jnp.where(col >= row, 1.0, 0.0).astype(BF16)
    last_in = jnp.where(col // BLOCK == row // BLOCK, 1.0, 0.0).astype(BF16)

    def hd(h):
        return slice(h * DK, (h + 1) * DK)

    def hv(h):
        return slice(h * DV, (h + 1) * DV)

    loads[0].wait()
    g_parts = pieces(g_ref[...], 3)
    span_buf[...] = sum(nn(tri, part_) for part_ in g_parts)
    c_buf[...] = sum(nn(tri_in, part_) for part_ in g_parts)
    total = span_buf[tokens - 1 : tokens, :]
    decay = jnp.exp(total)

    def scatter_copy(d, m, h):
        return pltpu.make_async_remote_copy(
            src_ref=a_out.at[d, m, h], dst_ref=a_in.at[d, x, h],
            send_sem=a_send.at[d, m, h], recv_sem=a_recv.at[d, x, h],
            device_id={"sp": z * nx + m}, device_id_type=MESH)

    def scatter_wait(d, h):
        for m in range(nx):
            @pl.when(m != x)
            def _():
                pltpu.make_async_remote_copy(
                    src_ref=a_out.at[d, m, h], dst_ref=a_in.at[d, m, h],
                    send_sem=a_send.at[d, m, h], recv_sem=a_recv.at[d, m, h],
                    device_id={"sp": z * nx + m}, device_id_type=MESH).wait_recv()

    def give(d, h, totals):
        for m in range(nx):
            a_out[d, m, h, :dvx, :] = totals[m * dvx : (m + 1) * dvx]
            a_out[d, m, h, dvx:, :] = jnp.broadcast_to(decay[:, hd(h)], (8, DK))
        for m in range(nx):
            @pl.when(m != x)
            def _():
                scatter_copy(d, m, h).start()

            @pl.when(m == x)
            def _():
                a_in[d, m, h] = a_out[d, m, h]

    loads[1].wait()
    q_all = q_ref[...].astype(F32) * scale
    q_span = (q_all * jnp.exp(span_buf[...])).astype(BF16)
    loads[2].wait()
    for h in range(heads):
        adjoint = tn(o_ref[:, hv(h)], q_span[:, hd(h)])
        if h == 0:
            pl.semaphore_wait(barrier, nx - 1 + nz - 1 + ntp - 1)
        give(1, h, adjoint)

    for load in loads[3:]:
        load.wait()
    k_all = k_ref[...].astype(F32)
    k_far = jnp.exp(total - span_buf[...])
    k_span = (k_all * k_far).astype(BF16)
    for h in range(heads):
        v_buf[:, hv(h)] = nn(x_ref[...], w_ref[:, hv(h)]).astype(BF16)
        give(0, h, tn(v_buf[:, hv(h)], k_span[:, hd(h)]))

    def order(d):
        return range(nx) if d == 0 else range(nx - 1, -1, -1)

    def plane_copy(dz):
        return pltpu.make_async_remote_copy(
            src_ref=z_out, dst_ref=z_in.at[z],
            send_sem=z_send.at[dz], recv_sem=z_recv.at[z],
            device_id={"sp": (z + dz) * nx + x}, device_id_type=MESH)

    def composite(d, h, rows_):
        acc, dec = None, None
        for m in order(d):
            local, rate = a_in[d, m, h, rows_, :], a_in[d, m, h, dvx : dvx + 1, :]
            acc = local if acc is None else local + rate * acc
            dec = rate if dec is None else rate * dec
        return acc, dec

    for h in range(heads):
        scatter_wait(1, h)

    def forward_start():
        for h in range(heads):
            scatter_wait(0, h)
            acc, dec = composite(0, h, slice(0, dvx))
            z_out[h, :dvx, :] = acc
            z_out[h, dvx:, :] = jnp.broadcast_to(dec, (8, DK))
        for dz in range(1, nz):
            @pl.when(z + dz < nz)
            def _():
                plane_copy(dz).start()

    @pl.when(z < nz - 1)
    def _():
        forward_start()

    half_v = dvx // 2

    def chain_copy(c):
        return pltpu.make_async_remote_copy(
            src_ref=h_out.at[c], dst_ref=h_in.at[c],
            send_sem=h_send.at[c], recv_sem=h_recv.at[c],
            device_id={"sp": (z - 1) * nx + x}, device_id_type=MESH)

    def piece_copy(m, c):
        return pltpu.make_async_remote_copy(
            src_ref=b_out.at[m, c], dst_ref=b_in.at[x, c],
            send_sem=b_send.at[m, c], recv_sem=b_recv.at[x, c],
            device_id={"sp": z * nx + m}, device_id_type=MESH)

    for c in range(2 * heads):
        h, rows_ = c // 2, slice(c % 2 * half_v, (c % 2 + 1) * half_v)
        acc, dec = composite(1, h, rows_)

        @pl.when(z == nz - 1)
        def _():
            h_in[c] = jnp.zeros((half_v, DK), F32)

        @pl.when(z < nz - 1)
        def _():
            chain_copy(c).wait_recv()

        enter = h_in[c]

        @pl.when(z > 0)
        def _():
            h_out[c] = acc + dec * enter
            chain_copy(c).start()

        for m in order(1):
            b_out[m, c] = enter
            enter = a_in[1, m, h, rows_, :] + a_in[1, m, h, dvx : dvx + 1, :] * enter
        for m in range(nx):
            @pl.when(m != x)
            def _():
                piece_copy(m, c).start()

            @pl.when(m == x)
            def _():
                b_in[m, c] = b_out[m, c]

    @pl.when(z == nz - 1)
    def _():
        for h in range(heads):
            scatter_wait(0, h)

    cum = c_buf[...]
    block_end = sum(nn(last_in, part_) for part_ in g_parts)
    k_tail = jnp.exp(block_end - cum)
    grow = jnp.exp(cum)
    qg_buf[...] = (q_all * grow).astype(BF16)
    ks_buf[...] = (k_all * jnp.exp(-cum)).astype(BF16)
    kt_buf[...] = (k_all * k_tail).astype(BF16)
    st_buf[...] = jnp.zeros_like(st_buf)

    def adjoint_step(step, carry):
        rows = pl.ds(pl.multiple_of((blocks - 1 - step) * BLOCK, BLOCK), BLOCK)
        for h in range(heads):
            keep = jnp.exp(c_buf[rows, hd(h)][BLOCK - 1 :])
            adjoint = st_buf[1, h]
            narrow = adjoint.astype(BF16)
            kp_buf[rows, hd(h)] = nn(v_buf[rows, hv(h)], narrow)
            vp_buf[rows, hv(h)] = nt(kt_buf[rows, hd(h)], narrow)
            st_buf[1, h] = keep * adjoint + tn(o_ref[rows, hv(h)], qg_buf[rows, hd(h)])
        return carry

    def state_step(step, carry):
        rows = pl.ds(pl.multiple_of(step * BLOCK, BLOCK), BLOCK)
        for h in range(heads):
            keep = jnp.exp(c_buf[rows, hd(h)][BLOCK - 1 :])
            state = st_buf[0, h]
            y_buf[rows, hd(h)] = nn(o_ref[rows, hv(h)], state.astype(BF16))
            st_buf[0, h] = keep * state + tn(v_buf[rows, hv(h)], kt_buf[rows, hd(h)])
        return carry

    lax.fori_loop(0, blocks, adjoint_step, 0)

    for h in range(heads):
        dots = jnp.where(inside, nt(qg_buf[:, hd(h)], ks_buf[:, hd(h)]), 0.0).astype(BF16)
        vp_buf[:, hv(h)] += tn(dots, o_ref[:, hv(h)])

    depth = x_ref.shape[1]
    for at in range(0, depth, 256):
        xt_buf[at : at + 256, :] = x_ref[:, at : at + 256].T

    def member_copy(m):
        return pltpu.make_async_remote_copy(
            src_ref=c_out.at[m], dst_ref=c_in.at[x],
            send_sem=c_send.at[m], recv_sem=c_recv.at[x],
            device_id={"sp": z * nx + m}, device_id_type=MESH)

    def forward_spread():
        z_acc[...] = jnp.zeros_like(z_acc)
        for zp in range(nz):
            @pl.when(zp < z)
            def _():
                pltpu.make_async_remote_copy(
                    src_ref=z_out, dst_ref=z_in.at[zp],
                    send_sem=z_send.at[0], recv_sem=z_recv.at[zp],
                    device_id={"sp": zp * nx + x}, device_id_type=MESH).wait_recv()
                for h in range(heads):
                    z_acc[h] = z_in[zp, h, :dvx, :] + z_in[zp, h, dvx : dvx + 1, :] * z_acc[h]
        for h in range(heads):
            acc = z_acc[h]
            for m in order(0):
                c_out[m, h] = acc
                acc = a_in[0, m, h, :dvx, :] + a_in[0, m, h, dvx : dvx + 1, :] * acc
        for m in range(nx):
            @pl.when(m != x)
            def _():
                member_copy(m).start()

            @pl.when(m == x)
            def _():
                c_in[m] = c_out[m]

    for h in range(heads):
        for m in range(nx):
            for c in (2 * h, 2 * h + 1):
                @pl.when(m != x)
                def _():
                    pltpu.make_async_remote_copy(
                        src_ref=b_out.at[m, c], dst_ref=b_in.at[m, c],
                        send_sem=b_send.at[m, c], recv_sem=b_recv.at[m, c],
                        device_id={"sp": z * nx + m}, device_id_type=MESH).wait_recv()
                at = m * dvx + c % 2 * half_v
                fr_buf[h, at : at + half_v, :] = b_in[m, c]
        narrow = fr_buf[h].astype(BF16)
        vg_buf[:, hv(h)] = (vp_buf[:, hv(h)] + nt(k_span[:, hd(h)], narrow)).astype(BF16)

    own = dw_ref.shape[0]
    half_r, half_c = own // 2, dw_ref.shape[1] // 2
    p = ring_place(z, x, nz, nx)
    ahead = ring_member((p + 1) % n, nz, nx)
    behind = ring_member((p + n - 1) % n, nz, nx)

    def share(d, u, owner):
        rows_ = pl.ds(pl.multiple_of(owner * own + u * half_r, half_r), half_r)
        return nn(xt_buf[rows_, :], vg_buf[:, d * half_c : (d + 1) * half_c])

    def ring_copy(step, d, u, src):
        return pltpu.make_async_remote_copy(
            src_ref=src, dst_ref=ring.at[step, d, u],
            send_sem=r_send.at[step, d, u], recv_sem=r_recv.at[step, d, u],
            device_id={"sp": ahead if d == 0 else behind}, device_id_type=MESH)

    def owner_at(step, d):
        return ring_member((p + n - step - 1) % n if d == 0 else (p + step + 1) % n, nz, nx)

    for u in range(2):
        for d in range(2):
            first[d, u] = share(d, u, owner_at(0, d))
            ring_copy(0, d, u, first.at[d, u]).start()

    lax.fori_loop(0, blocks, state_step, 0)
    for h in range(heads):
        dots = jnp.where(inside, nt(o_ref[:, hv(h)], v_buf[:, hv(h)]), 0.0).astype(BF16)
        y_buf[:, hd(h)] += nn(dots, ks_buf[:, hd(h)])
        k_grad = (
            k_tail[:, hd(h)] * kp_buf[:, hd(h)]
            + jnp.exp(-cum[:, hd(h)]) * tn(dots, qg_buf[:, hd(h)])
            + k_far[:, hd(h)] * nn(v_buf[:, hv(h)], fr_buf[h].astype(BF16))
        )
        kp_buf[:, hd(h)] = k_grad
        dk_ref[:, hd(h)] = k_grad.astype(BF16)
    forward_spread()

    def query_side():
        for m in range(nx):
            @pl.when(m != x)
            def _():
                pltpu.make_async_remote_copy(
                    src_ref=c_out.at[m], dst_ref=c_in.at[m],
                    send_sem=c_send.at[m], recv_sem=c_recv.at[m],
                    device_id={"sp": z * nx + m}, device_id_type=MESH).wait_recv()
        for h in range(heads):
            state_in = jnp.concatenate([c_in[m, h] for m in range(nx)], axis=0)
            q_side = q_ref[:, hd(h)].astype(F32) * scale
            k_side = k_ref[:, hd(h)].astype(F32)
            q_grad = jnp.exp(c_buf[:, hd(h)]) * y_buf[:, hd(h)] + jnp.exp(span_buf[:, hd(h)]) * nn(
                o_ref[:, hv(h)], state_in.astype(BF16)
            )
            dq_ref[:, hd(h)] = (q_grad * scale).astype(BF16)
            terms = q_side * q_grad - k_side * kp_buf[:, hd(h)]
            far = jnp.exp(span_buf[tokens - 1 : tokens, hd(h)])
            span_end = st_buf[0, h] + far * state_in
            carry = jnp.sum(fr_buf[h] * span_end, axis=0, keepdims=True)
            dg_ref[:, hd(h)] = sum(nn(upper, part_) for part_ in pieces(terms, 3)) + carry

    def ring_step(step, carry):
        for d in range(2):
            for u in range(2):
                part[d, u] = share(d, u, owner_at(step, d))
        for u in range(2):
            for d in range(2):
                ring_copy(step - 1, d, u, first.at[d, u]).wait_recv()
                ring[step - 1, d, u] += part[d, u]
                ring_copy(step, d, u, ring.at[step - 1, d, u]).start()

        @pl.when(step == 2)
        def _():
            query_side()

        return carry

    lax.fori_loop(1, n - 1, ring_step, 0)

    for d in range(2):
        for u in range(2):
            part[d, u] = share(d, u, me)
    for u in range(2):
        squares = 0.0
        for d in range(2):
            ring_copy(n - 2, d, u, first.at[d, u]).wait_recv()
            done = ring[n - 2, d, u] + part[d, u]
            dw_ref[u * half_r : (u + 1) * half_r, d * half_c : (d + 1) * half_c] = done
            for at in range(0, half_c, 128):
                squares = squares + done[:, at : at + 128] * done[:, at : at + 128]
        norm_out[u] = jnp.broadcast_to(jnp.sum(squares.T, axis=0, keepdims=True), (8, half_r))

    def norm_copy(off):
        return pltpu.make_async_remote_copy(
            src_ref=norm_out, dst_ref=norm_in.at[off],
            send_sem=n_send.at[off], recv_sem=n_recv.at[off],
            device_id={"tp": (mine + off) % ntp}, device_id_type=MESH)

    for off in range(1, ntp):
        norm_copy(off).start()

    for m in range(nx):
        @pl.when(m != x)
        def _():
            for h in range(heads):
                for d in range(2):
                    scatter_copy(d, m, h).wait_send()
            for c in range(2 * heads):
                piece_copy(m, c).wait_send()
            member_copy(m).wait_send()
    for dz in range(1, nz):
        @pl.when(z + dz < nz)
        def _():
            plane_copy(dz).wait_send()

    @pl.when(z > 0)
    def _():
        for c in range(2 * heads):
            chain_copy(c).wait_send()

    def sent(step, carry):
        for u in range(2):
            for d in range(2):
                ring_copy(step, d, u, first.at[d, u]).wait_send()
        return carry

    lax.fori_loop(0, n - 1, sent, 0)
    norms = norm_out[...]
    for off in range(1, ntp):
        norm_copy(off).wait()
        norms = norms + norm_in[off]
    rn_ref[...] = norms


def finish(*refs):
    for source, target in zip(refs[:4], refs[5:9]):
        target[...] = source[...]
    refs[9][...] = refs[4][:, :1]


def on_device(n, nx, ntp, block_input, queries, keys, w_value, log_decay, d_out):
    tokens, wide = queries.shape
    heads = wide // DK
    cols = w_value.shape[1]
    depth = block_input.shape[1]
    own = depth // n
    nz = n // nx
    dvx = DV // nx
    vm = pltpu.VMEM
    dma = pltpu.SemaphoreType.DMA
    out = pl.pallas_call(
        functools.partial(kernel, n, nx, ntp),
        out_shape=(
            jax.ShapeDtypeStruct((tokens, wide), BF16),
            jax.ShapeDtypeStruct((tokens, wide), BF16),
            jax.ShapeDtypeStruct((tokens, wide), F32),
            jax.ShapeDtypeStruct((own, cols), F32),
            jax.ShapeDtypeStruct((2, 8, own // 2), F32),
        ),
        in_specs=[pl.BlockSpec(memory_space=pltpu.HBM)] * 6,
        out_specs=(pl.BlockSpec(memory_space=vm),) * 5,
        scratch_shapes=[
            vm(block_input.shape, BF16),
            vm(queries.shape, BF16),
            vm(keys.shape, BF16),
            vm(w_value.shape, BF16),
            vm(log_decay.shape, F32),
            vm(d_out.shape, BF16),
            dma((6,)),
            vm((tokens, wide), F32),
            vm((tokens, wide), F32),
            vm((tokens, cols), BF16),
            vm((tokens, wide), BF16),
            vm((tokens, wide), BF16),
            vm((tokens, wide), BF16),
            vm((tokens, wide), F32),
            vm((tokens, wide), F32),
            vm((tokens, cols), F32),
            vm((2, heads, DV, DK), F32),
            vm((depth, tokens), BF16),
            vm((tokens, cols), BF16),
            vm((2, nx, heads, dvx + 8, DK), F32),
            vm((2, nx, heads, dvx + 8, DK), F32),
            vm((heads, dvx + 8, DK), F32),
            vm((nz, heads, dvx + 8, DK), F32),
            vm((heads, dvx, DK), F32),
            vm((nx, heads, dvx, DK), F32),
            vm((nx, heads, dvx, DK), F32),
            vm((2 * heads, dvx // 2, DK), F32),
            vm((2 * heads, dvx // 2, DK), F32),
            vm((nx, 2 * heads, dvx // 2, DK), F32),
            vm((nx, 2 * heads, dvx // 2, DK), F32),
            vm((heads, DV, DK), F32),
            vm((2, 2, own // 2, cols // 2), F32),
            vm((2, 2, own // 2, cols // 2), F32),
            vm((n - 1, 2, 2, own // 2, cols // 2), F32),
            vm((2, 8, own // 2), F32),
            vm((ntp, 2, 8, own // 2), F32),
            dma((2, nx, heads)),
            dma((2, nx, heads)),
            dma((nz,)),
            dma((nz,)),
            dma((nx,)),
            dma((nx,)),
            dma((2 * heads,)),
            dma((2 * heads,)),
            dma((nx, 2 * heads)),
            dma((nx, 2 * heads)),
            dma((n - 1, 2, 2)),
            dma((n - 1, 2, 2)),
            dma((ntp,)),
            dma((ntp,)),
        ],
        compiler_params=pltpu.CompilerParams(
            collective_id=0, has_side_effects=True, vmem_limit_bytes=60 * 1024 * 1024
        ),
    )(block_input, queries, keys, w_value, log_decay, d_out)
    final = pl.pallas_call(
        finish,
        out_shape=tuple(jax.ShapeDtypeStruct(a.shape, a.dtype) for a in out[:4])
        + (jax.ShapeDtypeStruct((2, 1, own // 2), F32),),
        in_specs=[pl.BlockSpec(memory_space=vm)] * 5,
        out_specs=(pl.BlockSpec(memory_space=vm),) * 5,
        compiler_params=pltpu.CompilerParams(vmem_limit_bytes=60 * 1024 * 1024),
    )(*out)
    return (*final[:4], final[4].reshape(-1))


def solution(mesh):
    n, ntp = mesh.shape["sp"], mesh.shape["tp"]
    nx = 1 << ((n.bit_length() - 1) // 2)
    placed = (
        P("sp", None),
        P("sp", "tp"),
        P("sp", "tp"),
        P(None, "tp"),
        P("sp", "tp"),
        P("sp", "tp"),
    )
    return jax.shard_map(
        functools.partial(on_device, n, nx, ntp),
        mesh=mesh,
        in_specs=placed,
        out_specs=(P("sp", "tp"), P("sp", "tp"), P("sp", "tp"), P("sp", "tp"), P("sp")),
        check_vma=False,
    )
```

```python
import functools

import jax
import jax.numpy as jnp
from jax import lax
from jax.experimental import pallas as pl
from jax.experimental.pallas import tpu as pltpu
from jax.sharding import PartitionSpec as P

DK = 128
DV = 256
BLOCK = 32
F32 = jnp.float32
BF16 = jnp.bfloat16
MESH = pl.DeviceIdType.MESH


def nn(left, right):
    return lax.dot_general(left, right, (((1,), (0,)), ((), ())), preferred_element_type=F32)


def nt(left, right):
    return lax.dot_general(left, right, (((1,), (1,)), ((), ())), preferred_element_type=F32)


def tn(left, right):
    return lax.dot_general(left, right, (((0,), (0,)), ((), ())), preferred_element_type=F32)


def pieces(value, count):
    parts = []
    for _ in range(count):
        part = value.astype(BF16)
        parts.append(part)
        value = value - part.astype(F32)
    return parts


def ring_place(z, x, nz, nx):
    r = nz - 1 - z
    across = jnp.where(r % 2 == 0, x - 1, nx - 1 - x)
    return jnp.where(x == 0, z, nz + r * (nx - 1) + across)


def ring_member(p, nz, nx):
    u = jnp.maximum(p - nz, 0)
    r = u // (nx - 1)
    w = u % (nx - 1)
    x = jnp.where(r % 2 == 0, 1 + w, nx - 1 - w)
    return jnp.where(p < nz, p * nx, (nz - 1 - r) * nx + x)


def kernel(
    n, nx, ntp,
    x_hbm, q_hbm, k_hbm, w_hbm, g_hbm, o_hbm,
    dq_ref, dk_ref, dg_ref, dw_ref, rn_ref,
    x_ref, q_ref, k_ref, w_ref, g_ref, o_ref, in_sem,
    c_buf, span_buf, v_buf, qg_buf, kt_buf, ks_buf, y_buf, kp_buf, vp_buf, st_buf, xt_buf, vg_buf,
    a_out, a_in, z_out, z_in, z_acc, c_out, c_in, h_out, h_in, b_out, b_in, fr_buf,
    first, part, ring, norm_out, norm_in,
    a_send, a_recv, z_send, z_recv, c_send, c_recv, h_send, h_recv, b_send, b_recv, r_send, r_recv, n_send, n_recv,
):
    nz = n // nx
    me = lax.axis_index("sp")
    mine = lax.axis_index("tp")
    z, x = me // nx, me % nx
    tokens, heads = q_ref.shape[0], q_ref.shape[1] // DK
    blocks = tokens // BLOCK
    dvx = DV // nx
    scale = DK ** (-0.5)
    loads = [
        pltpu.make_async_copy(source, target, in_sem.at[i])
        for i, (source, target) in enumerate(
            [(g_hbm, g_ref), (q_hbm, q_ref), (o_hbm, o_ref), (k_hbm, k_ref), (x_hbm, x_ref), (w_hbm, w_ref)]
        )
    ]
    for load in loads:
        load.start()
    barrier = pltpu.get_barrier_semaphore()
    for off in range(1, nx):
        pl.semaphore_signal(
            barrier, inc=1, device_id={"sp": z * nx + (x + off) % nx}, device_id_type=MESH)
    for off in range(1, nz):
        pl.semaphore_signal(
            barrier, inc=1, device_id={"sp": (z + off) % nz * nx + x}, device_id_type=MESH)
    for off in range(1, ntp):
        pl.semaphore_signal(barrier, inc=1, device_id={"tp": (mine + off) % ntp}, device_id_type=MESH)

    row = lax.broadcasted_iota(jnp.int32, (tokens, tokens), 0)
    col = lax.broadcasted_iota(jnp.int32, (tokens, tokens), 1)
    below = col <= row
    inside = below & (col // BLOCK == row // BLOCK)
    tri = jnp.where(below, 1.0, 0.0).astype(BF16)
    tri_in = jnp.where(inside, 1.0, 0.0).astype(BF16)
    upper = jnp.where(col >= row, 1.0, 0.0).astype(BF16)
    last_in = jnp.where(col // BLOCK == row // BLOCK, 1.0, 0.0).astype(BF16)

    def hd(h):
        return slice(h * DK, (h + 1) * DK)

    def hv(h):
        return slice(h * DV, (h + 1) * DV)

    loads[0].wait()
    g_parts = pieces(g_ref[...], 3)
    span_buf[...] = sum(nn(tri, part_) for part_ in g_parts)
    c_buf[...] = sum(nn(tri_in, part_) for part_ in g_parts)
    total = span_buf[tokens - 1 : tokens, :]
    decay = jnp.exp(total)

    def scatter_copy(d, m, h):
        return pltpu.make_async_remote_copy(
            src_ref=a_out.at[d, m, h], dst_ref=a_in.at[d, x, h],
            send_sem=a_send.at[d, m, h], recv_sem=a_recv.at[d, x, h],
            device_id={"sp": z * nx + m}, device_id_type=MESH)

    def scatter_wait(d, h):
        for m in range(nx):
            @pl.when(m != x)
            def _():
                pltpu.make_async_remote_copy(
                    src_ref=a_out.at[d, m, h], dst_ref=a_in.at[d, m, h],
                    send_sem=a_send.at[d, m, h], recv_sem=a_recv.at[d, m, h],
                    device_id={"sp": z * nx + m}, device_id_type=MESH).wait_recv()

    def give(d, h, totals):
        for m in range(nx):
            a_out[d, m, h, :dvx, :] = totals[m * dvx : (m + 1) * dvx]
            a_out[d, m, h, dvx:, :] = jnp.broadcast_to(decay[:, hd(h)], (8, DK))
        for m in range(nx):
            @pl.when(m != x)
            def _():
                scatter_copy(d, m, h).start()

            @pl.when(m == x)
            def _():
                a_in[d, m, h] = a_out[d, m, h]

    loads[1].wait()
    q_all = q_ref[...].astype(F32) * scale
    q_span = (q_all * jnp.exp(span_buf[...])).astype(BF16)
    loads[2].wait()
    for h in range(heads):
        adjoint = tn(o_ref[:, hv(h)], q_span[:, hd(h)])
        if h == 0:
            pl.semaphore_wait(barrier, nx - 1 + nz - 1 + ntp - 1)
        give(1, h, adjoint)

    for load in loads[3:]:
        load.wait()
    k_all = k_ref[...].astype(F32)
    k_far = jnp.exp(total - span_buf[...])
    k_span = (k_all * k_far).astype(BF16)
    for h in range(heads):
        v_buf[:, hv(h)] = nn(x_ref[...], w_ref[:, hv(h)]).astype(BF16)
        give(0, h, tn(v_buf[:, hv(h)], k_span[:, hd(h)]))

    def order(d):
        return range(nx) if d == 0 else range(nx - 1, -1, -1)

    def plane_copy(dz):
        return pltpu.make_async_remote_copy(
            src_ref=z_out, dst_ref=z_in.at[z],
            send_sem=z_send.at[dz], recv_sem=z_recv.at[z],
            device_id={"sp": (z + dz) * nx + x}, device_id_type=MESH)

    def composite(d, h, rows_):
        acc, dec = None, None
        for m in order(d):
            local, rate = a_in[d, m, h, rows_, :], a_in[d, m, h, dvx : dvx + 1, :]
            acc = local if acc is None else local + rate * acc
            dec = rate if dec is None else rate * dec
        return acc, dec

    def forward_start():
        for h in range(heads):
            scatter_wait(0, h)
            acc, dec = composite(0, h, slice(0, dvx))
            z_out[h, :dvx, :] = acc
            z_out[h, dvx:, :] = jnp.broadcast_to(dec, (8, DK))
        for dz in range(1, nz):
            @pl.when(z + dz < nz)
            def _():
                plane_copy(dz).start()

    @pl.when(z < nz - 1)
    def _():
        forward_start()

    half_v = dvx // 4

    def chain_copy(c):
        return pltpu.make_async_remote_copy(
            src_ref=h_out.at[c], dst_ref=h_in.at[c],
            send_sem=h_send.at[c], recv_sem=h_recv.at[c],
            device_id={"sp": (z - 1) * nx + x}, device_id_type=MESH)

    def piece_copy(m, c):
        return pltpu.make_async_remote_copy(
            src_ref=b_out.at[m, c], dst_ref=b_in.at[x, c],
            send_sem=b_send.at[m, c], recv_sem=b_recv.at[x, c],
            device_id={"sp": z * nx + m}, device_id_type=MESH)

    for c in range(4 * heads):
        h, rows_ = c // 4, slice(c % 4 * half_v, (c % 4 + 1) * half_v)
        if c % 4 == 0:
            scatter_wait(1, h)
        acc, dec = composite(1, h, rows_)

        @pl.when(z == nz - 1)
        def _():
            h_in[c] = jnp.zeros((half_v, DK), F32)

        @pl.when(z < nz - 1)
        def _():
            chain_copy(c).wait_recv()

        enter = h_in[c]

        @pl.when(z > 0)
        def _():
            h_out[c] = acc + dec * enter
            chain_copy(c).start()

        for m in order(1):
            b_out[m, c] = enter
            enter = a_in[1, m, h, rows_, :] + a_in[1, m, h, dvx : dvx + 1, :] * enter
        for m in range(nx):
            @pl.when(m != x)
            def _():
                piece_copy(m, c).start()

            @pl.when(m == x)
            def _():
                b_in[m, c] = b_out[m, c]

    @pl.when(z == nz - 1)
    def _():
        for h in range(heads):
            scatter_wait(0, h)

    cum = c_buf[...]
    block_end = sum(nn(last_in, part_) for part_ in g_parts)
    k_tail = jnp.exp(block_end - cum)
    grow = jnp.exp(cum)
    qg_buf[...] = (q_all * grow).astype(BF16)
    ks_buf[...] = (k_all * jnp.exp(-cum)).astype(BF16)
    kt_buf[...] = (k_all * k_tail).astype(BF16)
    st_buf[...] = jnp.zeros_like(st_buf)

    def adjoint_step(step, carry):
        rows = pl.ds(pl.multiple_of((blocks - 1 - step) * BLOCK, BLOCK), BLOCK)
        for h in range(heads):
            keep = jnp.exp(c_buf[rows, hd(h)][BLOCK - 1 :])
            adjoint = st_buf[1, h]
            narrow = adjoint.astype(BF16)
            kp_buf[rows, hd(h)] = nn(v_buf[rows, hv(h)], narrow)
            vp_buf[rows, hv(h)] = nt(kt_buf[rows, hd(h)], narrow)
            st_buf[1, h] = keep * adjoint + tn(o_ref[rows, hv(h)], qg_buf[rows, hd(h)])
        return carry

    def state_step(step, carry):
        rows = pl.ds(pl.multiple_of(step * BLOCK, BLOCK), BLOCK)
        for h in range(heads):
            keep = jnp.exp(c_buf[rows, hd(h)][BLOCK - 1 :])
            state = st_buf[0, h]
            y_buf[rows, hd(h)] = nn(o_ref[rows, hv(h)], state.astype(BF16))
            st_buf[0, h] = keep * state + tn(v_buf[rows, hv(h)], kt_buf[rows, hd(h)])
        return carry

    lax.fori_loop(0, blocks, adjoint_step, 0)

    for h in range(heads):
        dots = jnp.where(inside, nt(qg_buf[:, hd(h)], ks_buf[:, hd(h)]), 0.0).astype(BF16)
        vp_buf[:, hv(h)] += tn(dots, o_ref[:, hv(h)])

    depth = x_ref.shape[1]
    for at in range(0, depth, 256):
        xt_buf[at : at + 256, :] = x_ref[:, at : at + 256].T

    def member_copy(m):
        return pltpu.make_async_remote_copy(
            src_ref=c_out.at[m], dst_ref=c_in.at[x],
            send_sem=c_send.at[m], recv_sem=c_recv.at[x],
            device_id={"sp": z * nx + m}, device_id_type=MESH)

    def forward_spread():
        z_acc[...] = jnp.zeros_like(z_acc)
        for zp in range(nz):
            @pl.when(zp < z)
            def _():
                pltpu.make_async_remote_copy(
                    src_ref=z_out, dst_ref=z_in.at[zp],
                    send_sem=z_send.at[0], recv_sem=z_recv.at[zp],
                    device_id={"sp": zp * nx + x}, device_id_type=MESH).wait_recv()
                for h in range(heads):
                    z_acc[h] = z_in[zp, h, :dvx, :] + z_in[zp, h, dvx : dvx + 1, :] * z_acc[h]
        for h in range(heads):
            acc = z_acc[h]
            for m in order(0):
                c_out[m, h] = acc
                acc = a_in[0, m, h, :dvx, :] + a_in[0, m, h, dvx : dvx + 1, :] * acc
        for m in range(nx):
            @pl.when(m != x)
            def _():
                member_copy(m).start()

            @pl.when(m == x)
            def _():
                c_in[m] = c_out[m]

    for h in range(heads):
        for m in range(nx):
            for c in range(4 * h, 4 * (h + 1)):
                @pl.when(m != x)
                def _():
                    pltpu.make_async_remote_copy(
                        src_ref=b_out.at[m, c], dst_ref=b_in.at[m, c],
                        send_sem=b_send.at[m, c], recv_sem=b_recv.at[m, c],
                        device_id={"sp": z * nx + m}, device_id_type=MESH).wait_recv()
                at = m * dvx + c % 4 * half_v
                fr_buf[h, at : at + half_v, :] = b_in[m, c]
        narrow = fr_buf[h].astype(BF16)
        vg_buf[:, hv(h)] = (vp_buf[:, hv(h)] + nt(k_span[:, hd(h)], narrow)).astype(BF16)

    own = dw_ref.shape[0]
    half_r, half_c = own // 2, dw_ref.shape[1] // 2
    p = ring_place(z, x, nz, nx)
    ahead = ring_member((p + 1) % n, nz, nx)
    behind = ring_member((p + n - 1) % n, nz, nx)

    def share(d, u, owner):
        rows_ = pl.ds(pl.multiple_of(owner * own + u * half_r, half_r), half_r)
        return nn(xt_buf[rows_, :], vg_buf[:, d * half_c : (d + 1) * half_c])

    def ring_copy(step, d, u, src):
        return pltpu.make_async_remote_copy(
            src_ref=src, dst_ref=ring.at[step, d, u],
            send_sem=r_send.at[step, d, u], recv_sem=r_recv.at[step, d, u],
            device_id={"sp": ahead if d == 0 else behind}, device_id_type=MESH)

    def owner_at(step, d):
        return ring_member((p + n - step - 1) % n if d == 0 else (p + step + 1) % n, nz, nx)

    for u in range(2):
        for d in range(2):
            first[d, u] = share(d, u, owner_at(0, d))
            ring_copy(0, d, u, first.at[d, u]).start()

    lax.fori_loop(0, blocks, state_step, 0)
    for h in range(heads):
        dots = jnp.where(inside, nt(o_ref[:, hv(h)], v_buf[:, hv(h)]), 0.0).astype(BF16)
        y_buf[:, hd(h)] += nn(dots, ks_buf[:, hd(h)])
        k_grad = (
            k_tail[:, hd(h)] * kp_buf[:, hd(h)]
            + jnp.exp(-cum[:, hd(h)]) * tn(dots, qg_buf[:, hd(h)])
            + k_far[:, hd(h)] * nn(v_buf[:, hv(h)], fr_buf[h].astype(BF16))
        )
        kp_buf[:, hd(h)] = k_grad
        dk_ref[:, hd(h)] = k_grad.astype(BF16)
    forward_spread()

    def query_side():
        for m in range(nx):
            @pl.when(m != x)
            def _():
                pltpu.make_async_remote_copy(
                    src_ref=c_out.at[m], dst_ref=c_in.at[m],
                    send_sem=c_send.at[m], recv_sem=c_recv.at[m],
                    device_id={"sp": z * nx + m}, device_id_type=MESH).wait_recv()
        for h in range(heads):
            state_in = jnp.concatenate([c_in[m, h] for m in range(nx)], axis=0)
            q_side = q_ref[:, hd(h)].astype(F32) * scale
            k_side = k_ref[:, hd(h)].astype(F32)
            q_grad = jnp.exp(c_buf[:, hd(h)]) * y_buf[:, hd(h)] + jnp.exp(span_buf[:, hd(h)]) * nn(
                o_ref[:, hv(h)], state_in.astype(BF16)
            )
            dq_ref[:, hd(h)] = (q_grad * scale).astype(BF16)
            terms = q_side * q_grad - k_side * kp_buf[:, hd(h)]
            far = jnp.exp(span_buf[tokens - 1 : tokens, hd(h)])
            span_end = st_buf[0, h] + far * state_in
            carry = jnp.sum(fr_buf[h] * span_end, axis=0, keepdims=True)
            dg_ref[:, hd(h)] = sum(nn(upper, part_) for part_ in pieces(terms, 3)) + carry

    def ring_step(step, carry):
        for d in range(2):
            for u in range(2):
                part[d, u] = share(d, u, owner_at(step, d))
        for u in range(2):
            for d in range(2):
                ring_copy(step - 1, d, u, first.at[d, u]).wait_recv()
                ring[step - 1, d, u] += part[d, u]
                ring_copy(step, d, u, ring.at[step - 1, d, u]).start()

        @pl.when(step == 2)
        def _():
            query_side()

        return carry

    lax.fori_loop(1, n - 1, ring_step, 0)

    for d in range(2):
        for u in range(2):
            part[d, u] = share(d, u, me)
    for u in range(2):
        squares = 0.0
        for d in range(2):
            ring_copy(n - 2, d, u, first.at[d, u]).wait_recv()
            done = ring[n - 2, d, u] + part[d, u]
            dw_ref[u * half_r : (u + 1) * half_r, d * half_c : (d + 1) * half_c] = done
            for at in range(0, half_c, 128):
                squares = squares + done[:, at : at + 128] * done[:, at : at + 128]
        norm_out[u] = jnp.broadcast_to(jnp.sum(squares.T, axis=0, keepdims=True), (8, half_r))

    def norm_copy(off):
        return pltpu.make_async_remote_copy(
            src_ref=norm_out, dst_ref=norm_in.at[off],
            send_sem=n_send.at[off], recv_sem=n_recv.at[off],
            device_id={"tp": (mine + off) % ntp}, device_id_type=MESH)

    for off in range(1, ntp):
        norm_copy(off).start()

    for m in range(nx):
        @pl.when(m != x)
        def _():
            for h in range(heads):
                for d in range(2):
                    scatter_copy(d, m, h).wait_send()
            for c in range(4 * heads):
                piece_copy(m, c).wait_send()
            member_copy(m).wait_send()
    for dz in range(1, nz):
        @pl.when(z + dz < nz)
        def _():
            plane_copy(dz).wait_send()

    @pl.when(z > 0)
    def _():
        for c in range(4 * heads):
            chain_copy(c).wait_send()

    def sent(step, carry):
        for u in range(2):
            for d in range(2):
                ring_copy(step, d, u, first.at[d, u]).wait_send()
        return carry

    lax.fori_loop(0, n - 1, sent, 0)
    norms = norm_out[...]
    for off in range(1, ntp):
        norm_copy(off).wait()
        norms = norms + norm_in[off]
    rn_ref[...] = norms


def finish(*refs):
    for source, target in zip(refs[:4], refs[5:9]):
        target[...] = source[...]
    refs[9][...] = refs[4][:, :1]


def on_device(n, nx, ntp, block_input, queries, keys, w_value, log_decay, d_out):
    tokens, wide = queries.shape
    heads = wide // DK
    cols = w_value.shape[1]
    depth = block_input.shape[1]
    own = depth // n
    nz = n // nx
    dvx = DV // nx
    vm = pltpu.VMEM
    dma = pltpu.SemaphoreType.DMA
    out = pl.pallas_call(
        functools.partial(kernel, n, nx, ntp),
        out_shape=(
            jax.ShapeDtypeStruct((tokens, wide), BF16),
            jax.ShapeDtypeStruct((tokens, wide), BF16),
            jax.ShapeDtypeStruct((tokens, wide), F32),
            jax.ShapeDtypeStruct((own, cols), F32),
            jax.ShapeDtypeStruct((2, 8, own // 2), F32),
        ),
        in_specs=[pl.BlockSpec(memory_space=pltpu.HBM)] * 6,
        out_specs=(pl.BlockSpec(memory_space=vm),) * 5,
        scratch_shapes=[
            vm(block_input.shape, BF16),
            vm(queries.shape, BF16),
            vm(keys.shape, BF16),
            vm(w_value.shape, BF16),
            vm(log_decay.shape, F32),
            vm(d_out.shape, BF16),
            dma((6,)),
            vm((tokens, wide), F32),
            vm((tokens, wide), F32),
            vm((tokens, cols), BF16),
            vm((tokens, wide), BF16),
            vm((tokens, wide), BF16),
            vm((tokens, wide), BF16),
            vm((tokens, wide), F32),
            vm((tokens, wide), F32),
            vm((tokens, cols), F32),
            vm((2, heads, DV, DK), F32),
            vm((depth, tokens), BF16),
            vm((tokens, cols), BF16),
            vm((2, nx, heads, dvx + 8, DK), F32),
            vm((2, nx, heads, dvx + 8, DK), F32),
            vm((heads, dvx + 8, DK), F32),
            vm((nz, heads, dvx + 8, DK), F32),
            vm((heads, dvx, DK), F32),
            vm((nx, heads, dvx, DK), F32),
            vm((nx, heads, dvx, DK), F32),
            vm((4 * heads, dvx // 4, DK), F32),
            vm((4 * heads, dvx // 4, DK), F32),
            vm((nx, 4 * heads, dvx // 4, DK), F32),
            vm((nx, 4 * heads, dvx // 4, DK), F32),
            vm((heads, DV, DK), F32),
            vm((2, 2, own // 2, cols // 2), F32),
            vm((2, 2, own // 2, cols // 2), F32),
            vm((n - 1, 2, 2, own // 2, cols // 2), F32),
            vm((2, 8, own // 2), F32),
            vm((ntp, 2, 8, own // 2), F32),
            dma((2, nx, heads)),
            dma((2, nx, heads)),
            dma((nz,)),
            dma((nz,)),
            dma((nx,)),
            dma((nx,)),
            dma((4 * heads,)),
            dma((4 * heads,)),
            dma((nx, 4 * heads)),
            dma((nx, 4 * heads)),
            dma((n - 1, 2, 2)),
            dma((n - 1, 2, 2)),
            dma((ntp,)),
            dma((ntp,)),
        ],
        compiler_params=pltpu.CompilerParams(
            collective_id=0, has_side_effects=True, vmem_limit_bytes=60 * 1024 * 1024
        ),
    )(block_input, queries, keys, w_value, log_decay, d_out)
    final = pl.pallas_call(
        finish,
        out_shape=tuple(jax.ShapeDtypeStruct(a.shape, a.dtype) for a in out[:4])
        + (jax.ShapeDtypeStruct((2, 1, own // 2), F32),),
        in_specs=[pl.BlockSpec(memory_space=vm)] * 5,
        out_specs=(pl.BlockSpec(memory_space=vm),) * 5,
        compiler_params=pltpu.CompilerParams(vmem_limit_bytes=60 * 1024 * 1024),
    )(*out)
    return (*final[:4], final[4].reshape(-1))


def solution(mesh):
    n, ntp = mesh.shape["sp"], mesh.shape["tp"]
    nx = 1 << ((n.bit_length() - 1) // 2)
    placed = (
        P("sp", None),
        P("sp", "tp"),
        P("sp", "tp"),
        P(None, "tp"),
        P("sp", "tp"),
        P("sp", "tp"),
    )
    return jax.shard_map(
        functools.partial(on_device, n, nx, ntp),
        mesh=mesh,
        in_specs=placed,
        out_specs=(P("sp", "tp"), P("sp", "tp"), P("sp", "tp"), P("sp", "tp"), P("sp")),
        check_vma=False,
    )
```
